128 devices in a mesh: fs: 16 (over z, y), tp: 8 (over x, core).
Axes of the slice: x: 4, y: 4, z: 4, core: 2. Of those that a mesh axis runs over, the one named last changes fastest.
Arguments:
- weights_in: float32 [2, 2048, 5632], P(None, 'fs', 'tp'), may hold values from -6 to 6
- weights_mix: float32 [2048, 2048], P('fs', 'tp'), may hold values from -6 to 6
- momentum_in: float32 [2, 2048, 5632], P(None, 'fs', 'tp'), may hold values from -5 to 5
- momentum_mix: float32 [2048, 2048], P('fs', 'tp'), may hold values from -5 to 5
- grads_in: float32 [2, 2048, 5632], P(None, 'fs', 'tp'), may hold values from -5 to 5
- grads_mix: float32 [2048, 2048], P('fs', 'tp'), may hold values from -5 to 5
Outputs:
- momentum_in_next: float32 [2, 2048, 5632], P(None, 'fs', 'tp')
- momentum_mix_next: float32 [2048, 2048], P('fs', 'tp')
- weights_in_next: float32 [2, 2048, 5632], P(None, 'fs', 'tp')
- weights_mix_next: float32 [2048, 2048], P('fs', 'tp')
- update_in: float32 [2, 2048, 5632], P(None, 'fs', 'tp')
- update_mix: float32 [2048, 2048], P('fs', 'tp')
The draws below stay inside these ranges and needn't reach their ends.
All inputs are finite; a program needn't handle non-finite values.
Results may differ from the reference program's by a relative error of at most 0.0003.
Values sent between devices are 32-bit elements; how exact they have to be, the bound alone decides.
No kernel may reach another device: no remote copies, remote signals or barrier semaphores. Data moves between devices by JAX's collectives and lax.ppermute only.
A program may use at most 128 MiB of HBM per device.

```python
import math
import jax
import jax.numpy as jnp
from jax import lax

D = 2048
FF = 5632
ITERS = 3


def unit_field(key, shape):
    return jnp.clip(jax.random.normal(key, shape, jnp.float32), -5.0, 5.0)


def draw_momentum_in(key, part):
    return unit_field(jax.random.fold_in(key, 11), (2, D, FF))


def draw_momentum_mix(key, part):
    return unit_field(jax.random.fold_in(key, 12), (D, D))


def draw_grads_in(key, part):
    return unit_field(jax.random.fold_in(key, 13), (2, D, FF))


def draw_grads_mix(key, part):
    return unit_field(jax.random.fold_in(key, 14), (D, D))


def steps_of(key, dims, cuts, smallest, top_value):
    def one(position, parts):
        draws = jax.random.uniform(jax.random.fold_in(jax.random.fold_in(key, 6), position), (parts,), jnp.float32, smallest / len(cuts), top_value / len(cuts))
        return jnp.repeat(jnp.exp(draws), dims[position] // parts).reshape((-1,) + (1,) * (len(dims) - position - 1))

    gain = one(*cuts[0])
    for cut in cuts[1:]:
        gain = gain * one(*cut)
    return gain


def noise(rng, extent, deviation, limit, cuts=(), dtype=jnp.bfloat16):
    factor_of = steps_of(rng, extent, cuts, -0.22, 0.18) if cuts else 1.0
    values = jax.random.normal(rng, extent, jnp.float32) * deviation * factor_of
    return jnp.minimum(jnp.maximum(values, -limit), limit).astype(dtype)


def setup_inputs(seed: int = 0) -> dict:
    streams_of = jax.random.split(jax.random.key(seed), 7)
    weights_in = noise(streams_of[0], (2, D, FF), 1.0, 6.0, ((1, 16), (2, 8)), jnp.float32)
    weights_mix = noise(streams_of[1], (D, D), 1.0, 6.0, ((0, 16), (1, 8)), jnp.float32)
    momentum_in = draw_momentum_in(jax.random.fold_in(streams_of[6], 71), 0)
    momentum_mix = draw_momentum_mix(jax.random.fold_in(streams_of[6], 71), 0)
    grads_in = draw_grads_in(jax.random.fold_in(streams_of[6], 71), 0)
    grads_mix = draw_grads_mix(jax.random.fold_in(streams_of[6], 71), 0)
    return {"weights_in": weights_in, "weights_mix": weights_mix, "momentum_in": momentum_in, "momentum_mix": momentum_mix, "grads_in": grads_in, "grads_mix": grads_mix}


A_COEF = 3.4445
B_COEF = -4.775
C_COEF = 2.0315
MOMENTUM_DECAY = 0.95
STEP_RATE = 0.02
HIGH = lax.Precision.HIGHEST

def orthogonal(moment):
    row_total, col_total = moment.shape
    current = moment
    for iteration in range(ITERS):
        gram_sum = jnp.dot(current, current.T, precision=HIGH)
        if iteration == 0:
            scaling = 0.5 * lax.rsqrt(jnp.maximum(jnp.trace(gram_sum) / D, 1.0))
        else:
            scaling = jnp.float32(1.0)
        square = jnp.dot(gram_sum, gram_sum, precision=HIGH)
        poly_mat = scaling ** 2 * B_COEF * gram_sum + scaling ** 4 * C_COEF * square
        current = scaling * (A_COEF * current + jnp.dot(poly_mat, current, precision=HIGH))
    return current * math.sqrt(max(row_total, col_total))

def reference(weights_in, weights_mix, momentum_in, momentum_mix, grads_in, grads_mix):
    moment_in = MOMENTUM_DECAY * momentum_in + grads_in
    moment_mix = MOMENTUM_DECAY * momentum_mix + grads_mix
    step_in = jnp.stack([orthogonal(moment_in[0]), orthogonal(moment_in[1])])
    step_mix = orthogonal(moment_mix)
    return (moment_in, moment_mix, weights_in - STEP_RATE * step_in, weights_mix - STEP_RATE * step_mix, step_in, step_mix)
```

```python
import math

import jax
import jax.numpy as jnp
from jax import lax
from jax.experimental import pallas as pl
from jax.experimental.pallas import tpu as pltpu
from jax.sharding import Mesh, PartitionSpec as P

D = 2048
FF = 5632
A_COEF = 3.4445
B_COEF = -4.775
C_COEF = 2.0315
MOMENTUM_DECAY = 0.95
STEP_RATE = 0.02


RING = 4
PLANE = RING * RING
CORES = 2
ROWS = D // (PLANE * CORES)
BAND = D // PLANE
WINDOW = D // 2 + BAND
BLOCKS = WINDOW // BAND
HALF = ROWS // 2
COLS = FF // (2 * 16)
COLS_PAD = 192
MIX_COLS = D // 32
TILE = 512
REL = (0, -1, 1, 2)
BF = jnp.bfloat16
F32 = jnp.float32
VMEM_LIMIT = 60 * 1024 * 1024


def split(value):
    high = value.astype(BF)
    return high, (value - high.astype(F32)).astype(BF)


def dot(a, b):
    return jnp.dot(a, b, preferred_element_type=F32)


def shift(a, axis, by):
    return lax.ppermute(a, axis, [(i, (i + by) % RING) for i in range(RING)])


def swap(a):
    return lax.ppermute(a, "core", [(0, 1), (1, 0)])


def gram_body(pos, own, other, out_a, out_b, natural, left, right):
    y, x, core = pos[0], pos[1], pos[2]
    n_k = 2 * COLS_PAD
    pad = jnp.zeros((COLS_PAD - COLS, D), BF)
    for part, ref in enumerate((own, other)):
        base = part * COLS_PAD
        high, low = split(ref[...])
        for at, value in ((0, high), (n_k, low), (2 * n_k, high)):
            right[at + base : at + base + COLS, :D] = value
            right[at + base + COLS : at + base + COLS_PAD, :D] = pad
    right[:, D:] = right[:, : D // 2]
    fill = jnp.zeros((COLS_PAD - COLS, BAND), F32)
    for q in range(PLANE):
        cols = slice(q * BAND, (q + 1) * BAND)
        block = jnp.concatenate([own[:, cols], fill, other[:, cols], fill], axis=0)
        natural[cols, :] = block.T

    def chip(index, carry):
        outer, inner = index // RING, index % RING
        dy = jnp.where(outer == 3, 2, jnp.where(outer == 2, 3, outer))
        dx = jnp.where(inner == 3, 2, jnp.where(inner == 2, 3, inner))
        q = ((y + dy) % RING) * RING + (x + dx) % RING
        rows = pl.multiple_of(q * BAND + core * ROWS, ROWS)
        high, low = split(natural[pl.ds(rows, ROWS), :])
        left[:, :n_k] = high
        left[:, n_k : 2 * n_k] = high
        left[:, 2 * n_k :] = low
        start = pl.multiple_of(q * BAND, BAND)
        value = dot(left[...], right[:, pl.ds(start, WINDOW)])
        out_a[outer, inner] = value[:HALF]
        out_b[inner, outer] = value[HALF:]
        return carry

    lax.fori_loop(0, PLANE, chip, 0)


def gram_partials(pos, own, other):
    shape = jax.ShapeDtypeStruct((RING, RING, HALF, WINDOW), F32)
    return pl.pallas_call(
        gram_body,
        out_shape=(shape, shape),
        in_specs=[
            pl.BlockSpec(memory_space=pltpu.SMEM),
            pl.BlockSpec(memory_space=pltpu.VMEM),
            pl.BlockSpec(memory_space=pltpu.VMEM),
        ],
        out_specs=(pl.BlockSpec(memory_space=pltpu.VMEM),) * 2,
        scratch_shapes=[
            pltpu.VMEM((D, 2 * COLS_PAD), F32),
            pltpu.VMEM((ROWS, 6 * COLS_PAD), BF),
            pltpu.VMEM((6 * COLS_PAD, D + D // 2), BF),
        ],
        compiler_params=pltpu.CompilerParams(vmem_limit_bytes=VMEM_LIMIT),
        name="gram_partials",
    )(pos, own, other)


def ring_reduce(chunks, axis):
    half = chunks.shape[1] // 2
    from_prev = shift(chunks[3][:half], axis, 1)
    from_next = shift(chunks[3][half:], axis, -1)
    up = jnp.concatenate([chunks[1][:half] + from_prev, chunks[1][half:]])
    down = jnp.concatenate([chunks[2][:half], chunks[2][half:] + from_next])
    return chunks[0] + shift(up, axis, 1) + shift(down, axis, -1)


def ring_gather(own, axis):
    half = own.shape[0] // 2
    prev = shift(own, axis, 1)
    following = shift(own, axis, -1)
    far_a = shift(prev[:half], axis, 1)
    far_b = shift(following[half:], axis, -1)
    return own, prev, following, far_a, far_b


def stack_pieces(pieces):
    own, prev, following, far_a, far_b = pieces
    return jnp.stack([own, prev, following, jnp.concatenate([far_a, far_b])])


def plane_gather(rows):
    first = ring_gather(rows[:HALF], "x")
    second = ring_gather(rows[HALF:], "y")
    parts = ring_gather(stack_pieces(first), "y") + ring_gather(stack_pieces(second), "x")
    return parts + tuple(swap(p) for p in parts)


def piece_table():
    table = []
    for other in range(2):
        for half in range(2):
            for which, (rel, entries) in enumerate(
                ((0, range(4)), (-1, range(4)), (1, range(4)), (2, range(2)), (2, range(2, 4)))
            ):
                for at, entry in enumerate(entries):
                    dy, dx = (rel, REL[entry]) if half == 0 else (REL[entry], rel)
                    table.append((other * 10 + half * 5 + which, at, dy, dx, other, half))
    return table


PIECES = piece_table()


def fetch_pieces(pos, parts, store, sems):
    y, x, core = pos[0], pos[1], pos[2]
    copies = []
    for n, (array, at, dy, dx, other, half) in enumerate(PIECES):
        q = ((y + dy + RING) % RING) * RING + (x + dx + RING) % RING
        which = 1 - core if other else core
        start = pl.multiple_of(which * ROWS + half * HALF, HALF)
        copies.append(
            pltpu.make_async_copy(
                parts[array].at[at], store.at[q, pl.ds(start, HALF), :], sems.at[n]
            )
        )
    for c in copies:
        c.start()
    for c in copies:
        c.wait()


def assemble(store, ghi, glo, factor):
    def band(i, carry):
        rows = pl.multiple_of(i * BAND, BAND)
        for k in range(BLOCKS):
            j = (i + k) % PLANE
            cols = pl.multiple_of(j * BAND, BAND)
            block = store[i, :, k * BAND : (k + 1) * BAND]
            if factor is not None:
                block = block * factor
            high, low = split(block)
            ghi[pl.ds(rows, BAND), pl.ds(cols, BAND)] = high
            glo[pl.ds(rows, BAND), pl.ds(cols, BAND)] = low
            if 0 < k < BLOCKS - 1:
                high, low = split(block.T)
                ghi[pl.ds(cols, BAND), pl.ds(rows, BAND)] = high
                glo[pl.ds(cols, BAND), pl.ds(rows, BAND)] = low
        return carry

    lax.fori_loop(0, PLANE, band, 0)


def trace_of(store):
    eye = lax.broadcasted_iota(jnp.int32, (BAND, BAND), 0) == lax.broadcasted_iota(
        jnp.int32, (BAND, BAND), 1
    )
    total = jnp.zeros((BAND, BAND), F32)
    for i in range(PLANE):
        total = total + jnp.where(eye, store[i, :, :BAND], 0.0)
    return jnp.sum(total)


def product(both, ghi, glo, out):
    m = out.shape[0]

    def tile(j, carry):
        cols = pl.ds(pl.multiple_of(j * TILE, TILE), TILE)
        upper = dot(both[...], ghi[:, cols])
        lower = dot(both[:m, :], glo[:, cols])
        out[:, cols] = upper[:m] + (upper[m:] + lower)
        return carry

    lax.fori_loop(0, D // TILE, tile, 0)


def set_both(both, value):
    m = value.shape[0]
    high, low = split(value)
    both[:m, :] = high
    both[m:, :] = low


def apply_poly(value, both, tmp, ghi, glo):
    set_both(both, value[...])
    product(both, ghi, glo, tmp)
    first = tmp[...]
    value[...] = A_COEF * value[...] + B_COEF * first
    set_both(both, first)
    product(both, ghi, glo, tmp)
    value[...] = value[...] + C_COEF * tmp[...]


def next_gram_body(pos, *refs):
    parts, refs = refs[:20], refs[20:]
    rows_out, ghi_out, glo_out, scale_out = refs[:4]
    store, ghi, glo, both, value, tmp, sems, out_sems = refs[4:]
    y, x, core = pos[0], pos[1], pos[2]
    fetch_pieces(pos, parts, store, sems)
    scale = 0.5 * lax.rsqrt(jnp.full((1, BAND), jnp.maximum(trace_of(store) / D, 1.0), F32))
    scale_out[...] = jnp.broadcast_to(scale, scale_out.shape)
    assemble(store, ghi, glo, scale * scale)
    saves = [
        pltpu.make_async_copy(ghi, ghi_out, out_sems.at[0]),
        pltpu.make_async_copy(glo, glo_out, out_sems.at[1]),
    ]
    for c in saves:
        c.start()
    q = y * RING + x
    start = pl.multiple_of(q * BAND + core * ROWS, ROWS)
    value[...] = ghi[pl.ds(start, ROWS), :].astype(F32) + glo[pl.ds(start, ROWS), :].astype(F32)
    apply_poly(value, both, tmp, ghi, glo)
    apply_poly(value, both, tmp, ghi, glo)
    for k in range(BLOCKS):
        cols = pl.multiple_of(((q + k) % PLANE) * BAND, BAND)
        rows_out[:, k * BAND : (k + 1) * BAND] = value[:, pl.ds(cols, BAND)]
    for c in saves:
        c.wait()


def matrix_scratch(m):
    return [
        pltpu.VMEM((PLANE, BAND, WINDOW), F32),
        pltpu.VMEM((D, D), BF),
        pltpu.VMEM((D, D), BF),
        pltpu.VMEM((2 * m, D), BF),
        pltpu.VMEM((m, D), F32),
        pltpu.VMEM((m, D), F32),
    ]


def next_gram(pos, parts):
    matrix = jax.ShapeDtypeStruct((D, D), BF)
    return pl.pallas_call(
        next_gram_body,
        out_shape=(
            jax.ShapeDtypeStruct((ROWS, WINDOW), F32),
            matrix,
            matrix,
            jax.ShapeDtypeStruct((8, BAND), F32),
        ),
        in_specs=[pl.BlockSpec(memory_space=pltpu.SMEM)]
        + [pl.BlockSpec(memory_space=pl.ANY)] * 20,
        out_specs=(
            pl.BlockSpec(memory_space=pltpu.VMEM),
            pl.BlockSpec(memory_space=pl.ANY),
            pl.BlockSpec(memory_space=pl.ANY),
            pl.BlockSpec(memory_space=pltpu.VMEM),
        ),
        scratch_shapes=matrix_scratch(ROWS)
        + [pltpu.SemaphoreType.DMA((len(PIECES),)), pltpu.SemaphoreType.DMA((2,))],
        compiler_params=pltpu.CompilerParams(vmem_limit_bytes=VMEM_LIMIT),
        name="next_gram",
    )(pos, *parts)


def first_step_body(x_in, ghi, glo, scale, out, both, tmp):
    out[...] = x_in[...] * scale[0:1, 0:1]
    apply_poly(out, both, tmp, ghi, glo)


def first_step(x_t, ghi, glo, scale):
    return pl.pallas_call(
        first_step_body,
        out_shape=jax.ShapeDtypeStruct((COLS, D), F32),
        in_specs=[pl.BlockSpec(memory_space=pltpu.VMEM)] * 4,
        out_specs=pl.BlockSpec(memory_space=pltpu.VMEM),
        scratch_shapes=[pltpu.VMEM((2 * COLS, D), BF), pltpu.VMEM((COLS, D), F32)],
        compiler_params=pltpu.CompilerParams(vmem_limit_bytes=VMEM_LIMIT),
        name="first_step",
    )(x_t, ghi, glo, scale)


def last_steps_body(pos, x_in, *refs):
    parts, refs = refs[:20], refs[20:]
    out, store, ghi, glo, both, value, tmp, sems = refs
    fetch_pieces(pos, parts, store, sems)
    assemble(store, ghi, glo, None)
    value[...] = x_in[...]
    apply_poly(value, both, tmp, ghi, glo)
    out[...] = A_COEF * value[...]

    def next_power(n, carry):
        set_both(both, value[...])
        product(both, ghi, glo, tmp)
        value[...] = tmp[...]

        def step(_, inner):
            apply_poly(value, both, tmp, ghi, glo)
            return inner

        lax.fori_loop(0, 2, step, 0)
        out[...] = out[...] + jnp.where(n == 0, B_COEF, C_COEF) * value[...]
        return carry

    lax.fori_loop(0, 2, next_power, 0)


def last_steps(pos, x_t, parts):
    return pl.pallas_call(
        last_steps_body,
        out_shape=jax.ShapeDtypeStruct((COLS, D), F32),
        in_specs=[
            pl.BlockSpec(memory_space=pltpu.SMEM),
            pl.BlockSpec(memory_space=pltpu.VMEM),
        ]
        + [pl.BlockSpec(memory_space=pl.ANY)] * 20,
        out_specs=pl.BlockSpec(memory_space=pltpu.VMEM),
        scratch_shapes=matrix_scratch(COLS) + [pltpu.SemaphoreType.DMA((len(PIECES),))],
        compiler_params=pltpu.CompilerParams(vmem_limit_bytes=VMEM_LIMIT),
        name="last_steps",
    )(pos, x_t, *parts)


def local(weights_in, weights_mix, momentum_in, momentum_mix, grads_in, grads_mix):
    y = lax.axis_index("y")
    x = lax.axis_index("x")
    core = lax.axis_index("core")
    pos = jnp.stack([y, x, core]).astype(jnp.int32)
    moment_in = MOMENTUM_DECAY * momentum_in + grads_in
    moment_mix = MOMENTUM_DECAY * momentum_mix + grads_mix
    rows = moment_in.shape[1]

    turned_in = moment_in.transpose(0, 2, 1).reshape(2, RING, COLS, rows)
    turned_mix = moment_mix.T.reshape(1, RING, MIX_COLS, rows)
    turned_mix = jnp.pad(turned_mix, ((0, 1), (0, 0), (0, COLS - MIX_COLS), (0, 0)))
    send = jnp.concatenate([turned_in, turned_mix]).reshape(PLANE, COLS, rows)
    got = lax.all_to_all(send, ("z", "y"), 0, 0, tiled=True)
    x_t = got.transpose(1, 0, 2).reshape(COLS, D)

    part_a, part_b = gram_partials(pos, x_t, swap(x_t))
    rows_a = ring_reduce(ring_reduce(part_a, "y"), "x")
    rows_b = ring_reduce(ring_reduce(part_b, "x"), "y")
    parts = plane_gather(jnp.concatenate([rows_a, rows_b]))
    gram_rows, ghi, glo, scale = next_gram(pos, parts)
    parts = plane_gather(gram_rows)
    x_t = first_step(x_t, ghi, glo, scale)
    x_t = last_steps(pos, x_t, parts)

    send = x_t.reshape(COLS, PLANE, rows).transpose(1, 0, 2)
    got = lax.all_to_all(send, ("z", "y"), 0, 0, tiled=True).reshape(RING, RING, COLS, rows)
    step_in = got[:2].reshape(2, RING * COLS, rows).transpose(0, 2, 1) * math.sqrt(max(D, FF))
    step_mix = got[2, :, :MIX_COLS].reshape(RING * MIX_COLS, rows).T * math.sqrt(D)
    return (
        moment_in,
        moment_mix,
        weights_in - STEP_RATE * step_in,
        weights_mix - STEP_RATE * step_mix,
        step_in,
        step_mix,
    )


def solution(mesh):
    fine = Mesh(mesh.devices.reshape(4, 4, 4, 2), ("z", "y", "x", "core"))
    whole = P(None, ("z", "y"), ("x", "core"))
    mix = P(("z", "y"), ("x", "core"))
    specs = (whole, mix, whole, mix, whole, mix)
    return jax.shard_map(local, mesh=fine, in_specs=specs, out_specs=specs, check_vma=False)
```

```python
import math

import jax
import jax.numpy as jnp
from jax import lax
from jax.experimental import pallas as pl
from jax.experimental.pallas import tpu as pltpu
from jax.sharding import Mesh, PartitionSpec as P

D = 2048
FF = 5632
A_COEF = 3.4445
B_COEF = -4.775
C_COEF = 2.0315
MOMENTUM_DECAY = 0.95
STEP_RATE = 0.02


RING = 4
PLANE = RING * RING
CORES = 2
ROWS = D // (PLANE * CORES)
BAND = D // PLANE
WINDOW = D // 2 + BAND
BLOCKS = WINDOW // BAND
COLS = FF // (2 * 16)
COLS_PAD = 192
MIX_COLS = D // 32
TILE = 512
BF = jnp.bfloat16
F32 = jnp.float32
VMEM_LIMIT = 60 * 1024 * 1024


def split(value):
    high = value.astype(BF)
    return high, (value - high.astype(F32)).astype(BF)


def dot(a, b):
    return jnp.dot(a, b, preferred_element_type=F32)


def shift(a, phase, by):
    pairs = []
    for y in range(RING):
        for x in range(RING):
            for core in range(CORES):
                to = (y, (x + by) % RING) if core == phase else ((y + by) % RING, x)
                pairs.append(((y * RING + x) * CORES + core, (to[0] * RING + to[1]) * CORES + core))
    return lax.ppermute(a, ("y", "x", "core"), pairs)


def swap(a):
    return lax.ppermute(a, "core", [(0, 1), (1, 0)])


def chip_at(pos, core, near, far):
    y, x = pos[0], pos[1]
    dy = jnp.where(core == 0, far, near)
    dx = jnp.where(core == 0, near, far)
    return ((y + dy + RING) % RING) * RING + (x + dx + RING) % RING


TO = (0, 1, -1, 2)
FROM = (0, -1, 1, 2)


def gram_body(pos, own, other, *refs):
    outs, (left, right, acc, sems) = refs[:7], refs[7:]
    core = pos[2]
    n_k = 2 * COLS_PAD
    pad = jnp.zeros((COLS_PAD - COLS, D), BF)
    for part, ref in enumerate((own, other)):
        base = part * COLS_PAD
        high, low = split(ref[...])
        for at, value in ((0, high), (n_k, low), (2 * n_k, high)):
            right[at + base : at + base + COLS, :D] = value
            right[at + base + COLS : at + base + COLS_PAD, :D] = pad
    right[:, D:] = right[:, : D // 2]
    fill = jnp.zeros((COLS_PAD - COLS, BAND), F32)
    for q in range(PLANE):
        cols = slice(q * BAND, (q + 1) * BAND)
        block = jnp.concatenate([own[:, cols], fill, other[:, cols], fill], axis=0).T
        high, low = split(jnp.where(core == 0, block[:ROWS], block[ROWS:]))
        rows = slice(q * ROWS, (q + 1) * ROWS)
        left[rows, :n_k] = high
        left[rows, n_k : 2 * n_k] = high
        left[rows, 2 * n_k :] = low

    def row_of_chips(y, carry):
        rows = pl.ds(pl.multiple_of(y * RING * ROWS, RING * ROWS), RING * ROWS)
        cols = pl.ds(pl.multiple_of(y * RING * BAND, RING * BAND), WINDOW + (RING - 1) * BAND)
        value = dot(left[rows, :], right[:, cols])
        for x in range(RING):
            acc[y * RING + x] = value[
                x * ROWS : (x + 1) * ROWS, x * BAND : x * BAND + WINDOW
            ]
        return carry

    lax.fori_loop(0, RING, row_of_chips, 0)
    copies = []
    for far, pair in ((2, (5, 6)), (1, (1, 2)), (-1, (3, 4)), (0, (0, 0))):
        for entry, near in enumerate(TO):
            out = outs[pair[entry // 2]]
            at = entry if far == 0 else entry % 2
            copies.append(
                pltpu.make_async_copy(
                    acc.at[chip_at(pos, core, near, far)], out.at[at], sems.at[len(copies)]
                )
            )
    for c in copies:
        c.start()
    for c in copies:
        c.wait()


def gram_partials(pos, own, other):
    shapes = [jax.ShapeDtypeStruct((n, ROWS, WINDOW), F32) for n in (4, 2, 2, 2, 2, 2, 2)]
    return pl.pallas_call(
        gram_body,
        out_shape=shapes,
        in_specs=[
            pl.BlockSpec(memory_space=pltpu.SMEM),
            pl.BlockSpec(memory_space=pltpu.VMEM),
            pl.BlockSpec(memory_space=pltpu.VMEM),
        ],
        out_specs=[pl.BlockSpec(memory_space=pl.ANY)] * 7,
        scratch_shapes=[
            pltpu.VMEM((D // CORES, 6 * COLS_PAD), BF),
            pltpu.VMEM((6 * COLS_PAD, D + D // 2), BF),
            pltpu.VMEM((PLANE, ROWS, WINDOW), F32),
            pltpu.SemaphoreType.DMA((PLANE,)),
        ],
        compiler_params=pltpu.CompilerParams(vmem_limit_bytes=VMEM_LIMIT),
        name="gram_partials",
    )(pos, own, other)


def plane_reduce(partials):
    own, up_lo, up_hi, down_lo, down_hi, far_lo, far_hi = partials
    via_up = shift(far_lo, 1, 1)
    via_down = shift(far_hi, 1, -1)
    from_up_hi = shift(up_hi, 1, 1)
    from_down_lo = shift(down_lo, 1, -1)
    from_up_lo = shift(up_lo + via_up, 1, 1)
    from_down_hi = shift(down_hi + via_down, 1, -1)
    lo = own[:2] + from_up_lo + from_down_lo
    hi = own[2:] + from_up_hi + from_down_hi
    far = shift(hi[1], 0, 2)
    up = shift(lo[1], 0, 1)
    down = shift(hi[0], 0, -1)
    return lo[0] + up + down + far


def plane_gather(rows, work=None):
    far = shift(rows, 0, 2)
    prev = shift(rows, 0, 1)
    following = shift(rows, 0, -1)
    if work is None:
        lo = jnp.stack([rows, prev])
        prev_lo = shift(lo, 1, 1)
        next_lo = shift(lo, 1, -1)
        hi = jnp.stack([following, far])
        next_hi = shift(hi, 1, -1)
        prev_hi = shift(hi, 1, 1)
        far_lo = shift(prev_lo, 1, 1)
        far_hi = shift(next_hi, 1, -1)
        parts = (lo, hi, prev_lo, prev_hi, next_lo, next_hi, far_lo, far_hi)
        return parts + tuple(swap(p) for p in parts), None
    own = jnp.stack([rows, prev, following, far])
    prev = shift(own, 1, 1)
    following = shift(own, 1, -1)
    result = work(own)
    (first, second), result = lax.optimization_barrier(((prev[:2], following[2:]), result))
    far_lo = shift(first, 1, 1)
    far_hi = shift(second, 1, -1)
    parts = (own, prev, following, far_lo, far_hi)
    return parts + tuple(swap(p) for p in parts), result


def pieces_of(arrays):
    table = []
    for other in range(2):
        for where, far in enumerate((0, -1, 1, 2)):
            for entry in range(RING):
                if arrays == 16:
                    place = (2 * where + entry // 2, entry % 2)
                elif where < 3:
                    place = (where, entry)
                else:
                    place = (3 + entry // 2, entry % 2)
                table.append((other * arrays // 2 + place[0], place[1], FROM[entry], far, other))
    return table


def offset_of(index):
    return jnp.where(index == 1, RING - 1, jnp.where(index == 2, 1, jnp.where(index == 3, 2, 0)))


def load_matrix(pos, parts, store, ghi, glo, sems):
    eye = lax.broadcasted_iota(jnp.int32, (BAND, BAND), 0) == lax.broadcasted_iota(
        jnp.int32, (BAND, BAND), 1
    )
    order = [n for i in range(PLANE) for n in (i, PLANE + (i % RING) * RING + i // RING)]
    pieces = pieces_of(len(parts))
    for n in order:
        array, at, near, far, other = pieces[n]
        core = 1 - pos[2] if other else pos[2]
        start = pl.multiple_of(core * ROWS, ROWS)
        pltpu.make_async_copy(
            parts[array].at[at],
            store.at[chip_at(pos, core, near, far), pl.ds(start, ROWS), :],
            sems.at[n],
        ).start()

    def band(n, total):
        outer, inner = n // RING, n % RING
        i = chip_at(pos, pos[2], offset_of(inner), offset_of(outer))
        for sem in (n, PLANE + inner * RING + outer):
            pltpu.make_async_copy(
                parts[0].at[0], store.at[i, pl.ds(0, ROWS), :], sems.at[sem]
            ).wait()
        rows = pl.ds(pl.multiple_of(i * BAND, BAND), BAND)
        for k in range(BLOCKS):
            cols = pl.ds(pl.multiple_of(((i + k) % PLANE) * BAND, BAND), BAND)
            block = store[i, :, k * BAND : (k + 1) * BAND]
            if k == 0:
                total = total + jnp.where(eye, block, 0.0)
            high, low = split(block)
            ghi[rows, cols] = high
            glo[rows, cols] = low
            if 0 < k < BLOCKS - 1:
                ghi[cols, rows] = high.T
                glo[cols, rows] = low.T
        return total

    return jnp.sum(lax.fori_loop(0, PLANE, band, jnp.zeros((BAND, BAND), F32)))


def triple(both, high, low):
    m = both.shape[0] // 2
    upper = dot(both[...], high)
    lower = dot(both[:m, :], low)
    return upper[:m] + (upper[m:] + lower)


def set_both(both, value):
    m = value.shape[0]
    high, low = split(value)
    both[:m, :] = high
    both[m:, :] = low


def chain(both, value, tmp, ghi, glo, count, coefs_of, after=None):
    set_both(both, value[...])

    def step(n, carry):
        alpha, beta, closes = coefs_of(n)
        tmp[...] = triple(both, ghi[...], glo[...])
        new = alpha * value[...] + beta * tmp[...]
        value[...] = new
        set_both(both, jnp.where(closes, new, tmp[...]))
        if after is not None:
            after(n)
        return carry

    lax.fori_loop(0, count, step, 0)


def next_gram_body(pos, *refs):
    parts, refs = refs[:-12], refs[-12:]
    rows_out, ghi_out, glo_out, scale_out = refs[:4]
    store, ghi, glo, both, value, tmp, sems, out_sems = refs[4:]
    core = pos[2]
    ssq = load_matrix(pos, parts, store, ghi, glo, sems)
    saves = [
        pltpu.make_async_copy(ghi, ghi_out, out_sems.at[0]),
        pltpu.make_async_copy(glo, glo_out, out_sems.at[1]),
    ]
    for c in saves:
        c.start()
    scale = 0.5 * lax.rsqrt(jnp.full((8, BAND), jnp.maximum(ssq / D, 1.0), F32))
    scale_out[...] = scale
    two = (scale * scale)[:1, :1]
    q = pos[0] * RING + pos[1]
    mine = pl.ds(pl.multiple_of(q * BAND + core * ROWS, ROWS), ROWS)
    value[...] = two * (ghi[mine, :].astype(F32) + glo[mine, :].astype(F32))

    def coefs_of(n):
        closes = n % 2 == 1
        alpha = jnp.where(closes, 1.0, A_COEF)
        return alpha, jnp.where(closes, C_COEF * two * two, B_COEF * two), closes

    chain(both, value, tmp, ghi, glo, 4, coefs_of)
    for k in range(BLOCKS):
        cols = pl.multiple_of(((q + k) % PLANE) * BAND, BAND)
        rows_out[:, k * BAND : (k + 1) * BAND] = value[:, pl.ds(cols, BAND)]
    for c in saves:
        c.wait()


def matrix_scratch(m):
    return [
        pltpu.VMEM((PLANE, BAND, WINDOW), F32),
        pltpu.VMEM((D, D), BF),
        pltpu.VMEM((D, D), BF),
        pltpu.VMEM((2 * m, D), BF),
        pltpu.VMEM((m, D), F32),
        pltpu.VMEM((m, D), F32),
    ]


def next_gram(pos, parts):
    matrix = jax.ShapeDtypeStruct((D, D), BF)
    return pl.pallas_call(
        next_gram_body,
        out_shape=(
            jax.ShapeDtypeStruct((ROWS, WINDOW), F32),
            matrix,
            matrix,
            jax.ShapeDtypeStruct((8, BAND), F32),
        ),
        in_specs=[pl.BlockSpec(memory_space=pltpu.SMEM)]
        + [pl.BlockSpec(memory_space=pl.ANY)] * len(parts),
        out_specs=(
            pl.BlockSpec(memory_space=pltpu.VMEM),
            pl.BlockSpec(memory_space=pl.ANY),
            pl.BlockSpec(memory_space=pl.ANY),
            pl.BlockSpec(memory_space=pltpu.VMEM),
        ),
        scratch_shapes=matrix_scratch(ROWS)
        + [pltpu.SemaphoreType.DMA((2 * PLANE,)), pltpu.SemaphoreType.DMA((2,))],
        compiler_params=pltpu.CompilerParams(vmem_limit_bytes=VMEM_LIMIT),
        name="next_gram",
    )(pos, *parts)


def first_step_body(x_in, scale_in, ghi_in, glo_in, out, ghi, glo, both, tmp, sems):
    copies = []
    for n in range(D // TILE):
        cols = pl.ds(n * TILE, TILE)
        for part, (source, target) in enumerate(((ghi_in, ghi), (glo_in, glo))):
            copies.append(
                pltpu.make_async_copy(
                    source.at[:, cols], target.at[:, cols], sems.at[2 * n + part]
                )
            )
    for c in copies:
        c.start()
    scale = scale_in[:1, :1]
    two = scale * scale
    out[...] = scale * x_in[...]
    set_both(both, out[...])
    for n in range(D // TILE):
        copies[2 * n].wait()
        copies[2 * n + 1].wait()
        cols = slice(n * TILE, (n + 1) * TILE)
        tmp[:, cols] = triple(both, ghi[:, cols], glo[:, cols])
    out[...] = A_COEF * out[...] + B_COEF * two * tmp[...]
    set_both(both, tmp[...])
    tmp[...] = triple(both, ghi[...], glo[...])
    out[...] = out[...] + (C_COEF * two * two) * tmp[...]


def first_step(x_t, ghi, glo, scale):
    return pl.pallas_call(
        first_step_body,
        out_shape=jax.ShapeDtypeStruct((COLS, D), F32),
        in_specs=[pl.BlockSpec(memory_space=pltpu.VMEM)] * 2
        + [pl.BlockSpec(memory_space=pl.ANY)] * 2,
        out_specs=pl.BlockSpec(memory_space=pltpu.VMEM),
        scratch_shapes=[
            pltpu.VMEM((D, D), BF),
            pltpu.VMEM((D, D), BF),
            pltpu.VMEM((2 * COLS, D), BF),
            pltpu.VMEM((COLS, D), F32),
            pltpu.SemaphoreType.DMA((2 * D // TILE,)),
        ],
        compiler_params=pltpu.CompilerParams(vmem_limit_bytes=VMEM_LIMIT),
        cost_estimate=pl.CostEstimate(
            flops=12 * COLS * D * D, bytes_accessed=4 * D * D, transcendentals=0
        ),
        name="first_step",
    )(x_t, scale, ghi, glo)


def last_steps_body(pos, x_in, *refs):
    parts, refs = refs[:-8], refs[-8:]
    out, store, ghi, glo, both, value, tmp, sems = refs
    load_matrix(pos, parts, store, ghi, glo, sems)
    value[...] = x_in[...]
    out[...] = jnp.zeros(out.shape, F32)

    def coefs_of(n):
        place = (n + 3) % 5
        closes = jnp.logical_and(place != 0, place % 2 == 0)
        alpha = jnp.where(place == 0, 0.0, jnp.where(closes, 1.0, A_COEF))
        return alpha, jnp.where(place == 0, 1.0, jnp.where(closes, C_COEF, B_COEF)), closes

    def after(n):
        @pl.when(n % 5 == 1)
        def _():
            part = jnp.where(n == 1, A_COEF, jnp.where(n == 6, B_COEF, C_COEF))
            for q in range(PLANE):
                out[q] = out[q] + part * value[:, q * BAND : (q + 1) * BAND]

    chain(both, value, tmp, ghi, glo, 12, coefs_of, after)


def last_steps(pos, x_t, parts):
    return pl.pallas_call(
        last_steps_body,
        out_shape=jax.ShapeDtypeStruct((PLANE, COLS, BAND), F32),
        in_specs=[
            pl.BlockSpec(memory_space=pltpu.SMEM),
            pl.BlockSpec(memory_space=pltpu.VMEM),
        ]
        + [pl.BlockSpec(memory_space=pl.ANY)] * len(parts),
        out_specs=pl.BlockSpec(memory_space=pltpu.VMEM),
        scratch_shapes=matrix_scratch(COLS) + [pltpu.SemaphoreType.DMA((2 * PLANE,))],
        compiler_params=pltpu.CompilerParams(vmem_limit_bytes=VMEM_LIMIT),
        name="last_steps",
    )(pos, x_t, *parts)


def local(weights_in, weights_mix, momentum_in, momentum_mix, grads_in, grads_mix):
    y = lax.axis_index("y")
    x = lax.axis_index("x")
    core = lax.axis_index("core")
    pos = jnp.stack([y, x, core]).astype(jnp.int32)
    moment_in = MOMENTUM_DECAY * momentum_in + grads_in
    moment_mix = MOMENTUM_DECAY * momentum_mix + grads_mix
    moment_in, moment_mix = lax.optimization_barrier((moment_in, moment_mix))
    rows = moment_in.shape[1]

    turned_in = moment_in.transpose(0, 2, 1).reshape(2, RING, COLS, rows)
    turned_mix = moment_mix.T.reshape(1, RING, MIX_COLS, rows)
    turned_mix = jnp.pad(turned_mix, ((0, 1), (0, 0), (0, COLS - MIX_COLS), (0, 0)))
    send = jnp.concatenate([turned_in, turned_mix]).reshape(PLANE, COLS, rows)
    got = lax.all_to_all(send, ("z", "y"), 0, 0, tiled=True)
    x_t = got.transpose(1, 0, 2).reshape(COLS, D)

    parts, _ = plane_gather(plane_reduce(gram_partials(pos, x_t, swap(x_t))))
    gram_rows, ghi, glo, scale = next_gram(pos, parts)

    def work(ready):
        source, _ = lax.optimization_barrier((x_t, ready))
        return first_step(source, ghi, glo, scale)

    parts, x_t = plane_gather(gram_rows, work)
    send = last_steps(pos, x_t, parts)
    got = lax.all_to_all(send, ("z", "y"), 0, 0, tiled=True).reshape(RING, RING, COLS, rows)
    step_in = got[:2].reshape(2, RING * COLS, rows).transpose(0, 2, 1) * math.sqrt(max(D, FF))
    step_mix = got[2, :, :MIX_COLS].reshape(RING * MIX_COLS, rows).T * math.sqrt(D)
    return (
        moment_in,
        moment_mix,
        weights_in - STEP_RATE * step_in,
        weights_mix - STEP_RATE * step_mix,
        step_in,
        step_mix,
    )


def solution(mesh):
    fine = Mesh(mesh.devices.reshape(4, 4, 4, 2), ("z", "y", "x", "core"))
    whole = P(None, ("z", "y"), ("x", "core"))
    mix = P(("z", "y"), ("x", "core"))
    specs = (whole, mix, whole, mix, whole, mix)
    return jax.shard_map(local, mesh=fine, in_specs=specs, out_specs=specs, check_vma=False)
```

```python
import math

import jax
import jax.numpy as jnp
from jax import lax
from jax.experimental import pallas as pl
from jax.experimental.layout import Layout, with_layout_constraint
from jax.experimental.pallas import tpu as pltpu
from jax.sharding import Mesh, PartitionSpec as P

D = 2048
FF = 5632
A_COEF = 3.4445
B_COEF = -4.775
C_COEF = 2.0315
MOMENTUM_DECAY = 0.95
STEP_RATE = 0.02


RING = 4
PLANE = RING * RING
CORES = 2
ROWS = D // (PLANE * CORES)
BAND = D // PLANE
WINDOW = D // 2 + BAND
BLOCKS = WINDOW // BAND
COLS = FF // (2 * 16)
COLS_PAD = 192
MIX_COLS = D // 32
TILE = 512
BF = jnp.bfloat16
F32 = jnp.float32
VMEM_LIMIT = 60 * 1024 * 1024


def split(value):
    high = value.astype(BF)
    return high, (value - high.astype(F32)).astype(BF)


def dot(a, b):
    return jnp.dot(a, b, preferred_element_type=F32)


def shift(a, phase, by):
    pairs = []
    for y in range(RING):
        for x in range(RING):
            for core in range(CORES):
                to = (y, (x + by) % RING) if core == phase else ((y + by) % RING, x)
                pairs.append(((y * RING + x) * CORES + core, (to[0] * RING + to[1]) * CORES + core))
    return lax.ppermute(a, ("y", "x", "core"), pairs)


def swap(a):
    return lax.ppermute(a, "core", [(0, 1), (1, 0)])


def chip_at(pos, core, near, far):
    y, x = pos[0], pos[1]
    dy = jnp.where(core == 0, far, near)
    dx = jnp.where(core == 0, near, far)
    return ((y + dy + RING) % RING) * RING + (x + dx + RING) % RING


TO = (0, 1, -1, 2)
FROM = (0, -1, 1, 2)


def gram_body(pos, own, other, *refs):
    outs, (left, right, acc, sems) = refs[:7], refs[7:]
    core = pos[2]
    n_k = 2 * COLS_PAD
    pad = jnp.zeros((COLS_PAD - COLS, D), BF)
    for part, ref in enumerate((own, other)):
        base = part * COLS_PAD
        high, low = split(ref[...])
        for at, value in ((0, high), (n_k, low), (2 * n_k, high)):
            right[at + base : at + base + COLS, :D] = value
            right[at + base + COLS : at + base + COLS_PAD, :D] = pad
    right[:, D:] = right[:, : D // 2]
    fill = jnp.zeros((COLS_PAD - COLS, BAND), F32)
    for q in range(PLANE):
        cols = slice(q * BAND, (q + 1) * BAND)
        block = jnp.concatenate([own[:, cols], fill, other[:, cols], fill], axis=0).T
        high, low = split(jnp.where(core == 0, block[:ROWS], block[ROWS:]))
        rows = slice(q * ROWS, (q + 1) * ROWS)
        left[rows, :n_k] = high
        left[rows, n_k : 2 * n_k] = high
        left[rows, 2 * n_k :] = low

    copies = []
    for far, pair in ((2, (5, 6)), (1, (1, 2)), (-1, (3, 4)), (0, (0, 0))):
        for entry, near in enumerate(TO):
            chip = chip_at(pos, core, near, far)
            target = outs[pair[entry // 2]].at[entry if far == 0 else entry % 2]
            copies.append(
                (chip, pltpu.make_async_copy(acc.at[chip], target, sems.at[len(copies)]))
            )

    def row_of_chips(y, carry):
        rows = pl.ds(pl.multiple_of(y * RING * ROWS, RING * ROWS), RING * ROWS)
        cols = pl.ds(pl.multiple_of(y * RING * BAND, RING * BAND), WINDOW + (RING - 1) * BAND)
        value = dot(left[rows, :], right[:, cols])
        for x in range(RING):
            acc[y * RING + x] = value[
                x * ROWS : (x + 1) * ROWS, x * BAND : x * BAND + WINDOW
            ]
        for chip, copy in copies:
            pl.when(chip // RING == y)(copy.start)
        return carry

    lax.fori_loop(0, RING, row_of_chips, 0)
    for _, copy in copies:
        copy.wait()


def gram_partials(pos, own, other):
    shapes = [jax.ShapeDtypeStruct((n, ROWS, WINDOW), F32) for n in (4, 2, 2, 2, 2, 2, 2)]
    return pl.pallas_call(
        gram_body,
        out_shape=shapes,
        in_specs=[
            pl.BlockSpec(memory_space=pltpu.SMEM),
            pl.BlockSpec(memory_space=pltpu.VMEM),
            pl.BlockSpec(memory_space=pltpu.VMEM),
        ],
        out_specs=[pl.BlockSpec(memory_space=pl.ANY)] * 7,
        scratch_shapes=[
            pltpu.VMEM((D // CORES, 6 * COLS_PAD), BF),
            pltpu.VMEM((6 * COLS_PAD, D + D // 2), BF),
            pltpu.VMEM((PLANE, ROWS, WINDOW), F32),
            pltpu.SemaphoreType.DMA((PLANE,)),
        ],
        compiler_params=pltpu.CompilerParams(vmem_limit_bytes=VMEM_LIMIT),
        name="gram_partials",
    )(pos, own, other)


def plane_reduce(partials):
    own, up_lo, up_hi, down_lo, down_hi, far_lo, far_hi = partials
    via_up = shift(far_lo, 1, 1)
    via_down = shift(far_hi, 1, -1)
    from_up_hi = shift(up_hi, 1, 1)
    from_down_lo = shift(down_lo, 1, -1)
    from_up_lo = shift(up_lo + via_up, 1, 1)
    from_down_hi = shift(down_hi + via_down, 1, -1)
    lo = own[:2] + from_up_lo + from_down_lo
    hi = own[2:] + from_up_hi + from_down_hi
    far = shift(hi[1], 0, 2)
    up = shift(lo[1], 0, 1)
    down = shift(hi[0], 0, -1)
    return lo[0] + up + down + far


def plane_gather(rows, work=None):
    far = shift(rows, 0, 2)
    prev = shift(rows, 0, 1)
    following = shift(rows, 0, -1)
    if work is None:
        lo = jnp.stack([rows, prev])
        prev_lo = shift(lo, 1, 1)
        next_lo = shift(lo, 1, -1)
        hi = jnp.stack([following, far])
        next_hi = shift(hi, 1, -1)
        prev_hi = shift(hi, 1, 1)
        far_lo = shift(prev_lo, 1, 1)
        far_hi = shift(next_hi, 1, -1)
        parts = (lo, hi, prev_lo, prev_hi, next_lo, next_hi, far_lo, far_hi)
        return parts + tuple(swap(p) for p in parts), None
    own = jnp.stack([rows, prev, following, far])
    prev = shift(own, 1, 1)
    following = shift(own, 1, -1)
    result = work(own)
    (first, second), result = lax.optimization_barrier(((prev[:2], following[2:]), result))
    far_lo = shift(first, 1, 1)
    far_hi = shift(second, 1, -1)
    parts = (own, prev, following, far_lo, far_hi)
    return parts + tuple(swap(p) for p in parts), result


def pieces_of(arrays):
    table = []
    for other in range(2):
        for where, far in enumerate((0, -1, 1, 2)):
            for entry in range(RING):
                if arrays == 16:
                    place = (2 * where + entry // 2, entry % 2)
                elif where < 3:
                    place = (where, entry)
                else:
                    place = (3 + entry // 2, entry % 2)
                table.append((other * arrays // 2 + place[0], place[1], FROM[entry], far, other))
    return table


def offset_of(index):
    return jnp.where(index == 1, RING - 1, jnp.where(index == 2, 1, jnp.where(index == 3, 2, 0)))


def load_matrix(pos, parts, store, ghi, glo, sems):
    eye = lax.broadcasted_iota(jnp.int32, (BAND, BAND), 0) == lax.broadcasted_iota(
        jnp.int32, (BAND, BAND), 1
    )
    order = [n for i in range(PLANE) for n in (i, PLANE + (i % RING) * RING + i // RING)]
    pieces = pieces_of(len(parts))
    for n in order:
        array, at, near, far, other = pieces[n]
        core = 1 - pos[2] if other else pos[2]
        start = pl.multiple_of(core * ROWS, ROWS)
        pltpu.make_async_copy(
            parts[array].at[at],
            store.at[chip_at(pos, core, near, far), pl.ds(start, ROWS), :],
            sems.at[n],
        ).start()

    def band(n, total):
        outer, inner = n // RING, n % RING
        i = chip_at(pos, pos[2], offset_of(inner), offset_of(outer))
        for sem in (n, PLANE + inner * RING + outer):
            pltpu.make_async_copy(
                parts[0].at[0], store.at[i, pl.ds(0, ROWS), :], sems.at[sem]
            ).wait()
        rows = pl.ds(pl.multiple_of(i * BAND, BAND), BAND)
        for k in range(BLOCKS):
            cols = pl.ds(pl.multiple_of(((i + k) % PLANE) * BAND, BAND), BAND)
            block = store[i, :, k * BAND : (k + 1) * BAND]
            if k == 0:
                total = total + jnp.where(eye, block, 0.0)
            high, low = split(block)
            ghi[rows, cols] = high
            glo[rows, cols] = low
            if 0 < k < BLOCKS - 1:
                ghi[cols, rows] = high.T
                glo[cols, rows] = low.T
        return total

    return jnp.sum(lax.fori_loop(0, PLANE, band, jnp.zeros((BAND, BAND), F32)))


def triple(both, high, low):
    m = both.shape[0] // 2
    upper = dot(both[...], high)
    lower = dot(both[:m, :], low)
    return upper[:m] + (upper[m:] + lower)


def set_both(both, value):
    m = value.shape[0]
    high, low = split(value)
    both[:m, :] = high
    both[m:, :] = low


def chain(both, value, tmp, ghi, glo, count, coefs_of, after=None):
    set_both(both, value[...])

    def step(n, carry):
        alpha, beta, closes = coefs_of(n)
        tmp[...] = triple(both, ghi[...], glo[...])
        new = alpha * value[...] + beta * tmp[...]
        value[...] = new
        set_both(both, jnp.where(closes, new, tmp[...]))
        if after is not None:
            after(n)
        return carry

    lax.fori_loop(0, count, step, 0)


def next_gram_body(pos, *refs):
    parts, refs = refs[:-12], refs[-12:]
    rows_out, ghi_out, glo_out, scale_out = refs[:4]
    store, ghi, glo, both, value, tmp, sems, out_sems = refs[4:]
    core = pos[2]
    ssq = load_matrix(pos, parts, store, ghi, glo, sems)
    saves = [
        pltpu.make_async_copy(ghi, ghi_out, out_sems.at[0]),
        pltpu.make_async_copy(glo, glo_out, out_sems.at[1]),
    ]
    for c in saves:
        c.start()
    scale = 0.5 * lax.rsqrt(jnp.full((8, BAND), jnp.maximum(ssq / D, 1.0), F32))
    scale_out[...] = scale
    two = (scale * scale)[:1, :1]
    q = pos[0] * RING + pos[1]
    mine = pl.ds(pl.multiple_of(q * BAND + core * ROWS, ROWS), ROWS)
    value[...] = two * (ghi[mine, :].astype(F32) + glo[mine, :].astype(F32))

    def coefs_of(n):
        closes = n % 2 == 1
        alpha = jnp.where(closes, 1.0, A_COEF)
        return alpha, jnp.where(closes, C_COEF * two * two, B_COEF * two), closes

    chain(both, value, tmp, ghi, glo, 4, coefs_of)
    for k in range(BLOCKS):
        cols = pl.multiple_of(((q + k) % PLANE) * BAND, BAND)
        rows_out[:, k * BAND : (k + 1) * BAND] = value[:, pl.ds(cols, BAND)]
    for c in saves:
        c.wait()


def matrix_scratch(m):
    return [
        pltpu.VMEM((PLANE, BAND, WINDOW), F32),
        pltpu.VMEM((D, D), BF),
        pltpu.VMEM((D, D), BF),
        pltpu.VMEM((2 * m, D), BF),
        pltpu.VMEM((m, D), F32),
        pltpu.VMEM((m, D), F32),
    ]


def next_gram(pos, parts):
    matrix = jax.ShapeDtypeStruct((D, D), BF)
    return pl.pallas_call(
        next_gram_body,
        out_shape=(
            jax.ShapeDtypeStruct((ROWS, WINDOW), F32),
            matrix,
            matrix,
            jax.ShapeDtypeStruct((8, BAND), F32),
        ),
        in_specs=[pl.BlockSpec(memory_space=pltpu.SMEM)]
        + [pl.BlockSpec(memory_space=pl.ANY)] * len(parts),
        out_specs=(
            pl.BlockSpec(memory_space=pltpu.VMEM),
            pl.BlockSpec(memory_space=pl.ANY),
            pl.BlockSpec(memory_space=pl.ANY),
            pl.BlockSpec(memory_space=pltpu.VMEM),
        ),
        scratch_shapes=matrix_scratch(ROWS)
        + [pltpu.SemaphoreType.DMA((2 * PLANE,)), pltpu.SemaphoreType.DMA((2,))],
        compiler_params=pltpu.CompilerParams(vmem_limit_bytes=VMEM_LIMIT),
        name="next_gram",
    )(pos, *parts)


def first_step_body(x_in, scale_in, ghi_in, glo_in, out, ghi, glo, both, tmp, sems):
    copies = []
    for n in range(D // TILE):
        cols = pl.ds(n * TILE, TILE)
        for part, (source, target) in enumerate(((ghi_in, ghi), (glo_in, glo))):
            copies.append(
                pltpu.make_async_copy(
                    source.at[:, cols], target.at[:, cols], sems.at[2 * n + part]
                )
            )
    for c in copies:
        c.start()
    scale = scale_in[:1, :1]
    two = scale * scale
    out[...] = scale * x_in[...]
    set_both(both, out[...])
    for n in range(D // TILE):
        copies[2 * n].wait()
        copies[2 * n + 1].wait()
        cols = slice(n * TILE, (n + 1) * TILE)
        tmp[:, cols] = triple(both, ghi[:, cols], glo[:, cols])
    out[...] = A_COEF * out[...] + B_COEF * two * tmp[...]
    set_both(both, tmp[...])
    tmp[...] = triple(both, ghi[...], glo[...])
    out[...] = out[...] + (C_COEF * two * two) * tmp[...]


def first_step(x_t, ghi, glo, scale):
    return pl.pallas_call(
        first_step_body,
        out_shape=jax.ShapeDtypeStruct((COLS, D), F32),
        in_specs=[pl.BlockSpec(memory_space=pltpu.VMEM)] * 2
        + [pl.BlockSpec(memory_space=pl.ANY)] * 2,
        out_specs=pl.BlockSpec(memory_space=pltpu.VMEM),
        scratch_shapes=[
            pltpu.VMEM((D, D), BF),
            pltpu.VMEM((D, D), BF),
            pltpu.VMEM((2 * COLS, D), BF),
            pltpu.VMEM((COLS, D), F32),
            pltpu.SemaphoreType.DMA((2 * D // TILE,)),
        ],
        compiler_params=pltpu.CompilerParams(vmem_limit_bytes=VMEM_LIMIT),
        cost_estimate=pl.CostEstimate(
            flops=12 * COLS * D * D, bytes_accessed=4 * D * D, transcendentals=0
        ),
        name="first_step",
    )(x_t, scale, ghi, glo)


def last_steps_body(pos, x_in, *refs):
    parts, refs = refs[:-8], refs[-8:]
    out, store, ghi, glo, both, value, tmp, sems = refs
    load_matrix(pos, parts, store, ghi, glo, sems)
    value[...] = x_in[...]
    out[...] = jnp.zeros(out.shape, F32)

    def coefs_of(n):
        place = (n + 3) % 5
        closes = jnp.logical_and(place != 0, place % 2 == 0)
        alpha = jnp.where(place == 0, 0.0, jnp.where(closes, 1.0, A_COEF))
        return alpha, jnp.where(place == 0, 1.0, jnp.where(closes, C_COEF, B_COEF)), closes

    def after(n):
        @pl.when(n % 5 == 1)
        def _():
            part = jnp.where(n == 1, A_COEF, jnp.where(n == 6, B_COEF, C_COEF))
            for q in range(PLANE):
                out[q] = out[q] + part * value[:, q * BAND : (q + 1) * BAND]

    chain(both, value, tmp, ghi, glo, 12, coefs_of, after)


def last_steps(pos, x_t, parts):
    return pl.pallas_call(
        last_steps_body,
        out_shape=jax.ShapeDtypeStruct((PLANE, COLS, BAND), F32),
        in_specs=[
            pl.BlockSpec(memory_space=pltpu.SMEM),
            pl.BlockSpec(memory_space=pltpu.VMEM),
        ]
        + [pl.BlockSpec(memory_space=pl.ANY)] * len(parts),
        out_specs=pl.BlockSpec(memory_space=pltpu.VMEM),
        scratch_shapes=matrix_scratch(COLS) + [pltpu.SemaphoreType.DMA((2 * PLANE,))],
        compiler_params=pltpu.CompilerParams(vmem_limit_bytes=VMEM_LIMIT),
        name="last_steps",
    )(pos, x_t, *parts)


def local(weights_in, weights_mix, momentum_in, momentum_mix, grads_in, grads_mix):
    y = lax.axis_index("y")
    x = lax.axis_index("x")
    core = lax.axis_index("core")
    pos = jnp.stack([y, x, core]).astype(jnp.int32)
    moment_in = MOMENTUM_DECAY * momentum_in + grads_in
    moment_mix = MOMENTUM_DECAY * momentum_mix + grads_mix
    moment_mix = with_layout_constraint(moment_mix, Layout(major_to_minor=(0, 1)))
    rows = moment_in.shape[1]

    turned_in = moment_in.transpose(0, 2, 1).reshape(2, RING, COLS, rows)
    turned_mix = moment_mix.T.reshape(1, RING, MIX_COLS, rows)
    turned_mix = jnp.pad(turned_mix, ((0, 1), (0, 0), (0, COLS - MIX_COLS), (0, 0)))
    send = jnp.concatenate([turned_in, turned_mix]).reshape(PLANE, COLS, rows)
    got = lax.all_to_all(send, ("z", "y"), 0, 0, tiled=True)
    x_t = got.transpose(1, 0, 2).reshape(COLS, D)

    parts, _ = plane_gather(plane_reduce(gram_partials(pos, x_t, swap(x_t))))
    gram_rows, ghi, glo, scale = next_gram(pos, parts)

    def work(ready):
        source, _ = lax.optimization_barrier((x_t, ready))
        return first_step(source, ghi, glo, scale)

    parts, x_t = plane_gather(gram_rows, work)
    send = last_steps(pos, x_t, parts)
    got = lax.all_to_all(send, ("z", "y"), 0, 0, tiled=True).reshape(RING, RING, COLS, rows)
    step_in = got[:2].reshape(2, RING * COLS, rows).transpose(0, 2, 1) * math.sqrt(max(D, FF))
    step_mix = got[2, :, :MIX_COLS].reshape(RING * MIX_COLS, rows).T * math.sqrt(D)
    step_mix = with_layout_constraint(step_mix, Layout(major_to_minor=(0, 1)))
    return (
        moment_in,
        moment_mix,
        weights_in - STEP_RATE * step_in,
        weights_mix - STEP_RATE * step_mix,
        step_in,
        step_mix,
    )


def solution(mesh):
    fine = Mesh(mesh.devices.reshape(4, 4, 4, 2), ("z", "y", "x", "core"))
    whole = P(None, ("z", "y"), ("x", "core"))
    mix = P(("z", "y"), ("x", "core"))
    specs = (whole, mix, whole, mix, whole, mix)
    return jax.shard_map(local, mesh=fine, in_specs=specs, out_specs=specs, check_vma=False)
```

```python
import math

import jax
import jax.numpy as jnp
from jax import lax
from jax.experimental import pallas as pl
from jax.experimental.layout import Layout, with_layout_constraint
from jax.experimental.pallas import tpu as pltpu
from jax.sharding import Mesh, PartitionSpec as P

D = 2048
FF = 5632
A_COEF = 3.4445
B_COEF = -4.775
C_COEF = 2.0315
MOMENTUM_DECAY = 0.95
STEP_RATE = 0.02


RING = 4
PLANE = RING * RING
CORES = 2
ROWS = D // (PLANE * CORES)
BAND = D // PLANE
WINDOW = D // 2 + BAND
BLOCKS = WINDOW // BAND
COLS = FF // (2 * 16)
COLS_PAD = 192
MIX_COLS = D // 32
TILE = 512
BF = jnp.bfloat16
F32 = jnp.float32
VMEM_LIMIT = 60 * 1024 * 1024


def split(value):
    high = value.astype(BF)
    return high, (value - high.astype(F32)).astype(BF)


def dot(a, b):
    return jnp.dot(a, b, preferred_element_type=F32)


def shift(a, phase, by):
    pairs = []
    for y in range(RING):
        for x in range(RING):
            for core in range(CORES):
                to = (y, (x + by) % RING) if core == phase else ((y + by) % RING, x)
                pairs.append(((y * RING + x) * CORES + core, (to[0] * RING + to[1]) * CORES + core))
    return lax.ppermute(a, ("y", "x", "core"), pairs)


def swap(a):
    return lax.ppermute(a, "core", [(0, 1), (1, 0)])


def chip_at(pos, core, near, far):
    y, x = pos[0], pos[1]
    dy = jnp.where(core == 0, far, near)
    dx = jnp.where(core == 0, near, far)
    return ((y + dy + RING) % RING) * RING + (x + dx + RING) % RING


TO = (0, 1, -1, 2)
FROM = (0, -1, 1, 2)


def gram_body(pos, own, other, *refs):
    outs, (left, right, acc, sems) = refs[:7], refs[7:]
    core = pos[2]
    n_k = 2 * COLS_PAD
    pad = jnp.zeros((COLS_PAD - COLS, D), BF)
    for part, ref in enumerate((own, other)):
        base = part * COLS_PAD
        high, low = split(ref[...])
        for at, value in ((0, high), (n_k, low), (2 * n_k, high)):
            right[at + base : at + base + COLS, :D] = value
            right[at + base + COLS : at + base + COLS_PAD, :D] = pad
    right[:, D:] = right[:, : D // 2]
    fill = jnp.zeros((COLS_PAD - COLS, BAND), F32)
    for q in range(PLANE):
        cols = slice(q * BAND, (q + 1) * BAND)
        block = jnp.concatenate([own[:, cols], fill, other[:, cols], fill], axis=0).T
        high, low = split(jnp.where(core == 0, block[:ROWS], block[ROWS:]))
        rows = slice(q * ROWS, (q + 1) * ROWS)
        left[rows, :n_k] = high
        left[rows, n_k : 2 * n_k] = high
        left[rows, 2 * n_k :] = low

    copies = []
    for far, pair in ((2, (5, 6)), (1, (1, 2)), (-1, (3, 4)), (0, (0, 0))):
        for entry, near in enumerate(TO):
            chip = chip_at(pos, core, near, far)
            target = outs[pair[entry // 2]].at[entry if far == 0 else entry % 2]
            copies.append(
                (chip, pltpu.make_async_copy(acc.at[chip], target, sems.at[len(copies)]))
            )

    def row_of_chips(y, carry):
        rows = pl.ds(pl.multiple_of(y * RING * ROWS, RING * ROWS), RING * ROWS)
        cols = pl.ds(pl.multiple_of(y * RING * BAND, RING * BAND), WINDOW + (RING - 1) * BAND)
        value = dot(left[rows, :], right[:, cols])
        for x in range(RING):
            acc[y * RING + x] = value[
                x * ROWS : (x + 1) * ROWS, x * BAND : x * BAND + WINDOW
            ]
        for chip, copy in copies:
            pl.when(chip // RING == y)(copy.start)
        return carry

    lax.fori_loop(0, RING, row_of_chips, 0)
    for _, copy in copies:
        copy.wait()


def gram_partials(pos, own, other):
    shapes = [jax.ShapeDtypeStruct((n, ROWS, WINDOW), F32) for n in (4, 2, 2, 2, 2, 2, 2)]
    return pl.pallas_call(
        gram_body,
        out_shape=shapes,
        in_specs=[
            pl.BlockSpec(memory_space=pltpu.SMEM),
            pl.BlockSpec(memory_space=pltpu.VMEM),
            pl.BlockSpec(memory_space=pltpu.VMEM),
        ],
        out_specs=[pl.BlockSpec(memory_space=pl.ANY)] * 7,
        scratch_shapes=[
            pltpu.VMEM((D // CORES, 6 * COLS_PAD), BF),
            pltpu.VMEM((6 * COLS_PAD, D + D // 2), BF),
            pltpu.VMEM((PLANE, ROWS, WINDOW), F32),
            pltpu.SemaphoreType.DMA((PLANE,)),
        ],
        compiler_params=pltpu.CompilerParams(vmem_limit_bytes=VMEM_LIMIT),
        name="gram_partials",
    )(pos, own, other)


def plane_reduce(partials):
    own, up_lo, up_hi, down_lo, down_hi, far_lo, far_hi = partials
    via_up = shift(far_lo, 1, 1)
    via_down = shift(far_hi, 1, -1)
    from_up_hi = shift(up_hi, 1, 1)
    from_down_lo = shift(down_lo, 1, -1)
    from_up_lo = shift(up_lo + via_up, 1, 1)
    from_down_hi = shift(down_hi + via_down, 1, -1)
    lo = own[:2] + from_up_lo + from_down_lo
    hi = own[2:] + from_up_hi + from_down_hi
    far = shift(hi[1], 0, 2)
    up = shift(lo[1], 0, 1)
    down = shift(hi[0], 0, -1)
    return lo[0] + up + down + far


def plane_gather(rows, work=None):
    far = shift(rows, 0, 2)
    prev = shift(rows, 0, 1)
    following = shift(rows, 0, -1)
    if work is None:
        lo = jnp.stack([rows, prev])
        prev_lo = shift(lo, 1, 1)
        next_lo = shift(lo, 1, -1)
        hi = jnp.stack([following, far])
        next_hi = shift(hi, 1, -1)
        prev_hi = shift(hi, 1, 1)
        far_lo = shift(prev_lo, 1, 1)
        far_hi = shift(next_hi, 1, -1)
        parts = (lo, hi, prev_lo, prev_hi, next_lo, next_hi, far_lo, far_hi)
        return parts + tuple(swap(p) for p in parts), None
    own = jnp.stack([rows, prev, following, far])
    prev = shift(own, 1, 1)
    following = shift(own, 1, -1)
    result = work(own)
    (first, second), result = lax.optimization_barrier(((prev[:2], following[2:]), result))
    far_lo = shift(first, 1, 1)
    far_hi = shift(second, 1, -1)
    parts = (own, prev, following, far_lo, far_hi)
    return parts + tuple(swap(p) for p in parts), result


def pieces_of(arrays):
    table = []
    for other in range(2):
        for where, far in enumerate((0, -1, 1, 2)):
            for entry in range(RING):
                if arrays == 16:
                    place = (2 * where + entry // 2, entry % 2)
                elif where < 3:
                    place = (where, entry)
                else:
                    place = (3 + entry // 2, entry % 2)
                table.append((other * arrays // 2 + place[0], place[1], FROM[entry], far, other))
    return table


def offset_of(index):
    return jnp.where(index == 1, RING - 1, jnp.where(index == 2, 1, jnp.where(index == 3, 2, 0)))


def load_matrix(pos, parts, store, ghi, glo, sems):
    eye = lax.broadcasted_iota(jnp.int32, (BAND, BAND), 0) == lax.broadcasted_iota(
        jnp.int32, (BAND, BAND), 1
    )
    order = [n for i in range(PLANE) for n in (i, PLANE + (i % RING) * RING + i // RING)]
    pieces = pieces_of(len(parts))
    for n in order:
        array, at, near, far, other = pieces[n]
        core = 1 - pos[2] if other else pos[2]
        start = pl.multiple_of(core * ROWS, ROWS)
        pltpu.make_async_copy(
            parts[array].at[at],
            store.at[chip_at(pos, core, near, far), pl.ds(start, ROWS), :],
            sems.at[n],
        ).start()

    def band(n, total):
        outer, inner = n // RING, n % RING
        i = chip_at(pos, pos[2], offset_of(inner), offset_of(outer))
        for sem in (n, PLANE + inner * RING + outer):
            pltpu.make_async_copy(
                parts[0].at[0], store.at[i, pl.ds(0, ROWS), :], sems.at[sem]
            ).wait()
        rows = pl.ds(pl.multiple_of(i * BAND, BAND), BAND)
        for k in range(BLOCKS):
            cols = pl.ds(pl.multiple_of(((i + k) % PLANE) * BAND, BAND), BAND)
            block = store[i, :, k * BAND : (k + 1) * BAND]
            if k == 0:
                total = total + jnp.where(eye, block, 0.0)
            high, low = split(block)
            ghi[rows, cols] = high
            glo[rows, cols] = low
            if 0 < k < BLOCKS - 1:
                ghi[cols, rows] = high.T
                glo[cols, rows] = low.T
        return total

    return jnp.sum(lax.fori_loop(0, PLANE, band, jnp.zeros((BAND, BAND), F32)))


def triple(both, high, low):
    m = both.shape[0] // 2
    upper = dot(both[...], high)
    lower = dot(both[:m, :], low)
    return upper[:m] + (upper[m:] + lower)


def set_both(both, value):
    m = value.shape[0]
    high, low = split(value)
    both[:m, :] = high
    both[m:, :] = low


def chain(both, value, tmp, ghi, glo, count, coefs_of, after=None):
    set_both(both, value[...])

    def step(n, carry):
        alpha, beta, closes = coefs_of(n)
        tmp[...] = triple(both, ghi[...], glo[...])
        new = alpha * value[...] + beta * tmp[...]
        value[...] = new
        set_both(both, jnp.where(closes, new, tmp[...]))
        if after is not None:
            after(n)
        return carry

    lax.fori_loop(0, count, step, 0)


def next_gram_body(pos, *refs):
    parts, refs = refs[:-12], refs[-12:]
    rows_out, ghi_out, glo_out, scale_out = refs[:4]
    store, ghi, glo, both, value, tmp, sems, out_sems = refs[4:]
    core = pos[2]
    ssq = load_matrix(pos, parts, store, ghi, glo, sems)
    saves = [
        pltpu.make_async_copy(ghi, ghi_out, out_sems.at[0]),
        pltpu.make_async_copy(glo, glo_out, out_sems.at[1]),
    ]
    for c in saves:
        c.start()
    scale = 0.5 * lax.rsqrt(jnp.full((8, BAND), jnp.maximum(ssq / D, 1.0), F32))
    scale_out[...] = scale
    two = (scale * scale)[:1, :1]
    q = pos[0] * RING + pos[1]
    mine = pl.ds(pl.multiple_of(q * BAND + core * ROWS, ROWS), ROWS)
    value[...] = two * (ghi[mine, :].astype(F32) + glo[mine, :].astype(F32))

    def coefs_of(n):
        closes = n % 2 == 1
        alpha = jnp.where(closes, 1.0, A_COEF)
        return alpha, jnp.where(closes, C_COEF * two * two, B_COEF * two), closes

    chain(both, value, tmp, ghi, glo, 4, coefs_of)
    for k in range(BLOCKS):
        cols = pl.multiple_of(((q + k) % PLANE) * BAND, BAND)
        rows_out[:, k * BAND : (k + 1) * BAND] = value[:, pl.ds(cols, BAND)]
    for c in saves:
        c.wait()


def matrix_scratch(m):
    return [
        pltpu.VMEM((PLANE, BAND, WINDOW), F32),
        pltpu.VMEM((D, D), BF),
        pltpu.VMEM((D, D), BF),
        pltpu.VMEM((2 * m, D), BF),
        pltpu.VMEM((m, D), F32),
        pltpu.VMEM((m, D), F32),
    ]


def next_gram(pos, parts):
    matrix = jax.ShapeDtypeStruct((D, D), BF)
    return pl.pallas_call(
        next_gram_body,
        out_shape=(
            jax.ShapeDtypeStruct((ROWS, WINDOW), F32),
            matrix,
            matrix,
            jax.ShapeDtypeStruct((8, BAND), F32),
        ),
        in_specs=[pl.BlockSpec(memory_space=pltpu.SMEM)]
        + [pl.BlockSpec(memory_space=pl.ANY)] * len(parts),
        out_specs=(
            pl.BlockSpec(memory_space=pltpu.VMEM),
            pl.BlockSpec(memory_space=pl.ANY),
            pl.BlockSpec(memory_space=pl.ANY),
            pl.BlockSpec(memory_space=pltpu.VMEM),
        ),
        scratch_shapes=matrix_scratch(ROWS)
        + [pltpu.SemaphoreType.DMA((2 * PLANE,)), pltpu.SemaphoreType.DMA((2,))],
        compiler_params=pltpu.CompilerParams(vmem_limit_bytes=VMEM_LIMIT),
        name="next_gram",
    )(pos, *parts)


def first_step_body(x_in, scale_in, ghi_in, glo_in, out, ghi, glo, both, tmp, sems):
    copies = []
    for n in range(D // TILE):
        cols = pl.ds(n * TILE, TILE)
        for part, (source, target) in enumerate(((ghi_in, ghi), (glo_in, glo))):
            copies.append(
                pltpu.make_async_copy(
                    source.at[:, cols], target.at[:, cols], sems.at[2 * n + part]
                )
            )
    for c in copies:
        c.start()
    scale = scale_in[:1, :1]
    two = scale * scale
    out[...] = scale * x_in[...]
    set_both(both, out[...])
    for n in range(D // TILE):
        copies[2 * n].wait()
        copies[2 * n + 1].wait()
        cols = slice(n * TILE, (n + 1) * TILE)
        tmp[:, cols] = triple(both, ghi[:, cols], glo[:, cols])
    out[...] = A_COEF * out[...] + B_COEF * two * tmp[...]
    set_both(both, tmp[...])
    tmp[...] = triple(both, ghi[...], glo[...])
    out[...] = out[...] + (C_COEF * two * two) * tmp[...]


def first_step(x_t, ghi, glo, scale):
    return pl.pallas_call(
        first_step_body,
        out_shape=jax.ShapeDtypeStruct((COLS, D), F32),
        in_specs=[pl.BlockSpec(memory_space=pltpu.VMEM)] * 2
        + [pl.BlockSpec(memory_space=pl.ANY)] * 2,
        out_specs=pl.BlockSpec(memory_space=pltpu.VMEM),
        scratch_shapes=[
            pltpu.VMEM((D, D), BF),
            pltpu.VMEM((D, D), BF),
            pltpu.VMEM((2 * COLS, D), BF),
            pltpu.VMEM((COLS, D), F32),
            pltpu.SemaphoreType.DMA((2 * D // TILE,)),
        ],
        compiler_params=pltpu.CompilerParams(vmem_limit_bytes=VMEM_LIMIT),
        cost_estimate=pl.CostEstimate(
            flops=12 * COLS * D * D, bytes_accessed=4 * D * D, transcendentals=0
        ),
        name="first_step",
    )(x_t, scale, ghi, glo)


def last_steps_body(pos, x_in, *refs):
    parts, refs = refs[:-8], refs[-8:]
    out, store, ghi, glo, both, value, tmp, sems = refs
    load_matrix(pos, parts, store, ghi, glo, sems)
    value[...] = x_in[...]

    def coefs_of(n):
        place = (n + 3) % 5
        closes = jnp.logical_and(place != 0, place % 2 == 0)
        alpha = jnp.where(place == 0, 0.0, jnp.where(closes, 1.0, A_COEF))
        return alpha, jnp.where(place == 0, 1.0, jnp.where(closes, C_COEF, B_COEF)), closes

    def after(n):
        @pl.when(n == 1)
        def _():
            for q in range(PLANE):
                out[q] = A_COEF * value[:, q * BAND : (q + 1) * BAND]

        @pl.when(jnp.logical_or(n == 6, n == 11))
        def _():
            part = jnp.where(n == 6, B_COEF, C_COEF)
            for q in range(PLANE):
                out[q] = out[q] + part * value[:, q * BAND : (q + 1) * BAND]

    chain(both, value, tmp, ghi, glo, 12, coefs_of, after)


def last_steps(pos, x_t, parts):
    return pl.pallas_call(
        last_steps_body,
        out_shape=jax.ShapeDtypeStruct((PLANE, COLS, BAND), F32),
        in_specs=[
            pl.BlockSpec(memory_space=pltpu.SMEM),
            pl.BlockSpec(memory_space=pltpu.VMEM),
        ]
        + [pl.BlockSpec(memory_space=pl.ANY)] * len(parts),
        out_specs=pl.BlockSpec(memory_space=pltpu.VMEM),
        scratch_shapes=matrix_scratch(COLS) + [pltpu.SemaphoreType.DMA((2 * PLANE,))],
        compiler_params=pltpu.CompilerParams(vmem_limit_bytes=VMEM_LIMIT),
        name="last_steps",
    )(pos, x_t, *parts)


def local(weights_in, weights_mix, momentum_in, momentum_mix, grads_in, grads_mix):
    y = lax.axis_index("y")
    x = lax.axis_index("x")
    core = lax.axis_index("core")
    pos = jnp.stack([y, x, core]).astype(jnp.int32)
    moment_in = MOMENTUM_DECAY * momentum_in + grads_in
    moment_mix = MOMENTUM_DECAY * momentum_mix + grads_mix
    moment_mix = with_layout_constraint(moment_mix, Layout(major_to_minor=(0, 1)))
    rows = moment_in.shape[1]

    turned_in = moment_in.transpose(0, 2, 1).reshape(2, RING, COLS, rows)
    turned_mix = moment_mix.T.reshape(1, RING, MIX_COLS, rows)
    turned_mix = jnp.pad(turned_mix, ((0, 1), (0, 0), (0, COLS - MIX_COLS), (0, 0)))
    send = jnp.concatenate([turned_in, turned_mix]).reshape(PLANE, COLS, rows)
    got = lax.all_to_all(send, ("z", "y"), 0, 0, tiled=True)
    x_t = got.transpose(1, 0, 2).reshape(COLS, D)

    parts, _ = plane_gather(plane_reduce(gram_partials(pos, x_t, swap(x_t))))
    gram_rows, ghi, glo, scale = next_gram(pos, parts)

    def work(ready):
        source, _ = lax.optimization_barrier((x_t, ready))
        return first_step(source, ghi, glo, scale)

    parts, x_t = plane_gather(gram_rows, work)
    send = last_steps(pos, x_t, parts)
    got = lax.all_to_all(send, ("z", "y"), 0, 0, tiled=True).reshape(RING, RING, COLS, rows)
    step_in = got[:2].reshape(2, RING * COLS, rows).transpose(0, 2, 1) * math.sqrt(max(D, FF))
    step_mix = got[2, :, :MIX_COLS].reshape(RING * MIX_COLS, rows).T * math.sqrt(D)
    step_mix = with_layout_constraint(step_mix, Layout(major_to_minor=(0, 1)))
    return (
        moment_in,
        moment_mix,
        weights_in - STEP_RATE * step_in,
        weights_mix - STEP_RATE * step_mix,
        step_in,
        step_mix,
    )


def solution(mesh):
    fine = Mesh(mesh.devices.reshape(4, 4, 4, 2), ("z", "y", "x", "core"))
    whole = P(None, ("z", "y"), ("x", "core"))
    mix = P(("z", "y"), ("x", "core"))
    specs = (whole, mix, whole, mix, whole, mix)
    return jax.shard_map(local, mesh=fine, in_specs=specs, out_specs=specs, check_vma=False)
```
